32 devices in a mesh: kv: 16 (over z, y, x), tp: 2 (over core).
Axes of the slice: x: 2, y: 2, z: 4, core: 2. Of those that a mesh axis runs over, the one named last changes fastest.
Arguments:
- tokens: bfloat16 [4096, 2048], P('kv'), may hold values from -72 to 72
- w_query: bfloat16 [2048, 1024], P(None, 'tp'), may hold values from -0.125 to 0.125
- w_key: bfloat16 [2048, 1024], P(None, 'tp'), may hold values from -0.125 to 0.125
- w_value: bfloat16 [2048, 1024], P(None, 'tp'), may hold values from -0.125 to 0.125
- w_out: bfloat16 [1024, 2048], P('tp'), may hold values from -0.1875 to 0.1875
- chosen: int32 [64, 16], replicated, may hold values from -1 to 63, as said below
Outputs:
- mixed: bfloat16 [4096, 2048], P(('kv', 'tp'))
- log_sums: float32 [16, 4096], P('tp', 'kv')
The draws below stay inside these ranges and needn't reach their ends.
Inputs may be any that keep to these rules, and one draw needn't show every extreme that they name: `chosen`: row b begins with b itself, then lists distinct key blocks at most b, then holds -1 in its remaining entries. Taken together, the rows of the query blocks of one index of kv list at most 2 distinct blocks of the positions of any other index of kv, and exactly 2 for some pairs of indices in every draw.
All inputs are finite; a program needn't handle non-finite values.
Results may differ from the reference program's by a relative error of at most 0.03.
Values may be sent and summed in bfloat16 or wider, within the bound.
A program may use at most 64 MiB of HBM per device.

```python
import jax
import jax.numpy as jnp
from jax import lax

D = 2048
HEADS = 16
HEAD_DIM = 64
BLK = 64
SEL = 16
CAP = 2
TOK_DEV = 256
ATT = 1024
TOKENS = 4096
NBLK = 64
N_TP = 2


def draw_tokens(key, part):
    values = jnp.clip(jax.random.normal(key, (TOKENS, D), jnp.float32), -6.0, 6.0)
    return values.astype(jnp.bfloat16)


def draw_chosen(key, part):
    per_dev = TOK_DEV // BLK
    devices = NBLK // per_dev
    pair_key = jax.random.fold_in(key, 11)
    hot_key = jax.random.fold_in(key, 12)
    rank_key = jax.random.fold_in(key, 13)
    order_bits = jax.random.randint(pair_key, (devices, devices, per_dev), 0, 1 << 20) * per_dev + jnp.arange(per_dev)
    ordering = jnp.argsort(order_bits, axis=-1)[..., :CAP]
    picked_blocks = jnp.arange(devices)[None, :, None] * per_dev + ordering
    hotness = jax.random.randint(hot_key, (devices,), 0, 4)
    blocks = jnp.arange(NBLK)
    query_block = blocks[:, None]
    target = blocks[None, :]
    query_dev = query_block // per_dev
    target_dev = target // per_dev
    pair_table = jnp.any(picked_blocks[:, blocks // per_dev, :] == blocks[None, :, None], axis=-1)
    in_pair = pair_table[blocks // per_dev] & (target_dev < query_dev)
    same_dev = (target_dev == query_dev) & (target <= query_block)
    near_dev = (target_dev == query_dev - 1) | (target_dev == query_dev - devices // 2)
    tier_level = jnp.where(target == query_block, 3, jnp.where(same_dev | in_pair & near_dev, 2, 1))
    jitter = jax.random.randint(rank_key, (NBLK, NBLK), 0, 1 << 12)
    rating = ((tier_level * 4 + hotness[target_dev]) * 4096 + jitter) * NBLK + target
    rating = jnp.where(same_dev | in_pair, rating, -1 - target)
    values, position = lax.top_k(rating, SEL)
    return jnp.where(values >= 0, position, -1).astype(jnp.int32)


def level_of(stream_key, extent, split, smallest, high):
    gain = 1.0
    for dim, blocks in split:
        steps = jax.random.uniform(jax.random.fold_in(jax.random.fold_in(stream_key, 6), dim), (blocks,), jnp.float32, smallest / len(split), high / len(split))
        gain = gain * jnp.repeat(jnp.exp(steps), extent[dim] // blocks).reshape((-1,) + (1,) * (len(extent) - 1 - dim))
    return gain


def normal_values(stream_key, shape, deviation, reach, cuts=(), held_as=jnp.bfloat16):
    result = deviation * jax.random.normal(stream_key, shape, jnp.float32)
    if cuts:
        result = result * level_of(stream_key, shape, cuts, -0.22, 0.18)
    return jnp.clip(result, -reach, reach).astype(held_as)


def setup_inputs(seed: int = 0) -> dict:
    keys = jax.random.split(jax.random.key(seed), 7)
    tokens = draw_tokens(jax.random.fold_in(keys[6], 71), 0)
    w_query = normal_values(keys[1], (D, ATT), D ** -0.5, 0.125, ((1, 2),))
    w_key = normal_values(keys[2], (D, ATT), D ** -0.5, 0.125, ((1, 2),))
    w_value = normal_values(keys[3], (D, ATT), D ** -0.5, 0.125, ((1, 2),))
    w_out = normal_values(keys[4], (ATT, D), ATT ** -0.5, 0.1875, ((0, 2),))
    chosen = draw_chosen(jax.random.fold_in(keys[6], 71), 0)
    return dict(tokens=tokens, w_query=w_query, w_key=w_key, w_value=w_value, w_out=w_out, chosen=chosen)


rotary_base = 500000.0
masked_score = -1e30


def rotate(values, positions, head_count, head_size):
    half_size = head_size // 2
    inverse = rotary_base ** (-jnp.arange(half_size, dtype=jnp.float32) / half_size)
    angles = positions.astype(jnp.float32)[:, None, None] * inverse[None, None, :]
    cos_part = jnp.cos(angles)
    sin_part = jnp.sin(angles)
    grouped = values.reshape(values.shape[0], head_count, head_size)
    first_half = grouped[..., :half_size]
    second_half = grouped[..., half_size:]
    turned = jnp.concatenate([first_half * cos_part - second_half * sin_part, second_half * cos_part + first_half * sin_part], axis=-1)
    return turned.reshape(values.shape)


def reference(tokens, w_query, w_key, w_value, w_out, chosen):
    positions = jnp.arange(TOKENS)
    query = rotate(jnp.dot(tokens, w_query, preferred_element_type=jnp.float32), positions, HEADS, HEAD_DIM).astype(jnp.bfloat16)
    keys_all = rotate(jnp.dot(tokens, w_key, preferred_element_type=jnp.float32), positions, HEADS, HEAD_DIM).astype(jnp.bfloat16)
    values_all = jnp.dot(tokens, w_value, preferred_element_type=jnp.float32).astype(jnp.bfloat16)
    key_blocks = keys_all.reshape(NBLK, BLK, HEADS, HEAD_DIM)
    value_blocks = values_all.reshape(NBLK, BLK, HEADS, HEAD_DIM)
    query_blocks = query.reshape(NBLK, BLK, HEADS, HEAD_DIM)
    scaling = HEAD_DIM ** -0.5

    def one_block(inputs):
        query_rows, listed = inputs
        usable = listed >= 0
        safe_rows = jnp.maximum(listed, 0)
        picked_keys = key_blocks[safe_rows].reshape(SEL * BLK, HEADS, HEAD_DIM)
        picked_values = value_blocks[safe_rows].reshape(SEL * BLK, HEADS, HEAD_DIM)
        scores = jnp.einsum('qhd,khd->hqk', query_rows.astype(jnp.float32), picked_keys.astype(jnp.float32)) * scaling
        key_mask = jnp.broadcast_to(usable[:, None], (SEL, BLK)).reshape(SEL * BLK)
        scores = jnp.where(key_mask[None, None, :], scores, masked_score)
        row_max = jnp.max(scores, axis=-1)
        weights = jnp.where(key_mask[None, None, :], jnp.exp(scores - row_max[..., None]), 0.0)
        totals = jnp.sum(weights, axis=-1)
        rounded = lax.optimization_barrier(weights.astype(jnp.bfloat16)).astype(jnp.float32)
        summed = jnp.einsum('hqk,khd->qhd', rounded, picked_values.astype(jnp.float32))
        mixed_rows = (summed / jnp.transpose(totals)[:, :, None]).reshape(BLK, HEADS * HEAD_DIM).astype(jnp.bfloat16)
        return mixed_rows, row_max + jnp.log(totals)

    mixed_all, log_blocks = lax.map(one_block, (query_blocks, chosen))
    attended = mixed_all.reshape(TOKENS, HEADS * HEAD_DIM)
    log_sums = jnp.transpose(log_blocks, (1, 0, 2)).reshape(HEADS, TOKENS)
    group_width = HEADS * HEAD_DIM // N_TP
    output = jnp.zeros((TOKENS, D), jnp.float32)
    for group_index in range(N_TP):
        lower = group_index * group_width
        partial_sum = jnp.dot(attended[:, lower:lower + group_width], w_out[lower:lower + group_width], preferred_element_type=jnp.float32)
        output = output + lax.optimization_barrier(partial_sum.astype(jnp.bfloat16)).astype(jnp.float32)
    return output.astype(jnp.bfloat16), log_sums
```

```python
import functools

import jax
import jax.numpy as jnp
from jax import lax
from jax.experimental import pallas as pl
from jax.experimental.pallas import tpu as pltpu
from jax.sharding import PartitionSpec as P

HEAD_DIM = 64
BLK = 64
CAP = 2
LANES = 128
VMEM_LIMIT = 48 * 1024 * 1024

rotary_base = 500000.0
masked_score = -1e30


def in_vmem():
    return pl.BlockSpec(memory_space=pltpu.VMEM)


def in_smem():
    return pl.BlockSpec(memory_space=pltpu.SMEM)


def project_kernel(tiles, x_ref, wk_ref, wv_ref, wq_ref, cos_ref, sin_ref, kv_ref, q_ref):
    step = pl.program_id(0)
    half = HEAD_DIM // 2
    cos_part = cos_ref[...]
    sin_part = sin_ref[...]
    low = lax.broadcasted_iota(jnp.int32, cos_part.shape, 1) % HEAD_DIM < half

    def turned(values):
        parts = []
        for lane in range(0, values.shape[1], LANES):
            part = values[:, lane : lane + LANES]
            other = jnp.where(low, pltpu.roll(part, LANES - half, 1), pltpu.roll(part, half, 1))
            parts.append(part * cos_part + other * sin_part)
        return jnp.concatenate(parts, axis=1) if len(parts) > 1 else parts[0]

    @pl.when(step < tiles)
    def _():
        made = jnp.dot(x_ref[...], wk_ref[...], preferred_element_type=jnp.float32)
        kv_ref[0] = turned(made).astype(jnp.bfloat16)

    @pl.when((step >= tiles) & (step < 2 * tiles))
    def _():
        made = jnp.dot(x_ref[...], wv_ref[...], preferred_element_type=jnp.float32)
        kv_ref[0] = made.astype(jnp.bfloat16)

    @pl.when(step >= 2 * tiles)
    def _():
        made = jnp.dot(x_ref[...], wq_ref[...], preferred_element_type=jnp.float32)
        q_ref[...] = (turned(made).astype(jnp.bfloat16) * (HEAD_DIM**-0.5)).astype(jnp.bfloat16)


def exchange_kernel(
    layers, group, blocks, sel_ref, kv_ref, tab_ref, stage, col_send, col_recv, pl_send, pl_recv, own_sem
):
    chunks = kv_ref.shape[0]
    me = lax.axis_index("kv")
    z = lax.div(me, group)
    g = lax.rem(me, group)
    up = lax.rem(me + group, layers * group)
    down = lax.rem(me + (layers - 1) * group, layers * group)
    span = blocks * BLK

    barrier = pltpu.get_barrier_semaphore()
    peers = [z * group + lax.rem(g + d, group) for d in range(group)]
    for d in range(1, group):
        pl.semaphore_signal(barrier, inc=1, device_id={"kv": peers[d]}, device_id_type=pl.DeviceIdType.MESH)

    @pl.when(z < layers - 1)
    def _():
        pl.semaphore_signal(barrier, inc=1, device_id={"kv": up}, device_id_type=pl.DeviceIdType.MESH)

    @pl.when(z > 0)
    def _():
        pl.semaphore_signal(barrier, inc=1, device_id={"kv": down}, device_id_type=pl.DeviceIdType.MESH)

    pl.semaphore_wait(barrier, group - 1 + jnp.minimum(z, 1) + jnp.minimum(layers - 1 - z, 1))

    own = pltpu.make_async_copy(kv_ref, tab_ref.at[:, pl.ds(0, span)], own_sem)
    own.start()

    def column(t, ch):
        return tab_ref.at[ch, pl.ds(t * span, span)]

    def column_copy(t, ch):
        source = kv_ref.at[ch] if t == 0 else column(t, ch)
        return pltpu.make_async_remote_copy(
            src_ref=source,
            dst_ref=column(t + 1, ch),
            send_sem=col_send.at[t, ch],
            recv_sem=col_recv.at[t, ch],
            device_id={"kv": up},
            device_id_type=pl.DeviceIdType.MESH,
        )

    def plane_copy(d, t, ch):
        place = (layers * blocks + ((d - 1) * layers + t) * CAP) * BLK
        return pltpu.make_async_remote_copy(
            src_ref=stage.at[d - 1, t, ch],
            dst_ref=tab_ref.at[ch, pl.ds(place, CAP * BLK)],
            send_sem=pl_send.at[d - 1, t, ch],
            recv_sem=pl_recv.at[d - 1, t, ch],
            device_id={"kv": peers[d]},
            device_id_type=pl.DeviceIdType.MESH,
        )

    for t in range(layers):

        @pl.when(z >= t)
        def _():
            def one_chunk(ch, carry):
                if t > 0:
                    column_copy(t - 1, ch).wait_recv()
                if t < layers - 1:

                    @pl.when(z < layers - 1)
                    def _():
                        column_copy(t, ch).start()

                def hand_on(d):
                    for c in range(CAP):
                        index = sel_ref[peers[d], ((z - t) * group + g) * CAP + c]
                        picked = None
                        for i in range(blocks):
                            source = kv_ref if t == 0 else tab_ref
                            tile = source[ch, pl.ds(t * span + i * BLK, BLK), :]
                            picked = tile if picked is None else jnp.where(index == i, tile, picked)
                        stage[d - 1, t, ch, pl.ds(c * BLK, BLK), :] = picked
                    plane_copy(d, t, ch).start()

                for d in range(1, group):
                    if t == 0:
                        pl.when(g + d < group)(functools.partial(hand_on, d))
                    else:
                        hand_on(d)
                return carry

            lax.fori_loop(0, chunks, one_chunk, 0)

    own.wait()
    for t in range(layers):

        @pl.when(z >= t)
        def _():
            def one_chunk(ch, carry):
                if t < layers - 1:

                    @pl.when(z < layers - 1)
                    def _():
                        column_copy(t, ch).wait_send()

                for d in range(1, group):
                    if t == 0:
                        pl.when(g + d < group)(lambda d=d: plane_copy(d, t, ch).wait_send())
                        pl.when(g >= d)(lambda d=d: plane_copy(d, t, ch).wait_recv())
                    else:
                        plane_copy(d, t, ch).wait_send()
                        plane_copy(d, t, ch).wait_recv()
                return carry

            lax.fori_loop(0, chunks, one_chunk, 0)


def attend_kernel(
    layers, group, blocks, chosen_ref, slot_ref, q_ref, tab_ref, out_ref, log_ref, keys, values
):
    chunks = tab_ref.shape[0]
    wide = tab_ref.shape[2]
    entries = chosen_ref.shape[1]
    width = q_ref.shape[1]
    me = lax.axis_index("kv")
    z = lax.div(me, group)
    g = lax.rem(me, group)

    def one_block(r, carry):
        mine = me * blocks + r
        count = 0
        for s in range(entries):
            listed = chosen_ref[mine, s]
            count = count + jnp.where(listed >= 0, 1, 0)
            block = jnp.where(listed >= 0, listed, mine)
            owner = lax.div(block, blocks)
            t = z - lax.div(owner, group)
            d = lax.rem(g - lax.rem(owner, group) + group, group)
            row = jnp.where(
                d == 0,
                t * blocks + lax.rem(block, blocks),
                layers * blocks + ((d - 1) * layers + t) * CAP + slot_ref[me, block],
            )
            start = pl.multiple_of(row * BLK, BLK)
            for ch in range(chunks // 2):
                lanes = slice(ch * wide, (ch + 1) * wide)
                keys[s * BLK : (s + 1) * BLK, lanes] = tab_ref[ch, pl.ds(start, BLK), :]
                values[s * BLK : (s + 1) * BLK, lanes] = tab_ref[chunks // 2 + ch, pl.ds(start, BLK), :]
        rows = pl.ds(pl.multiple_of(r * BLK, BLK), BLK)
        first = lax.broadcasted_iota(jnp.int32, (BLK, LANES), 1) < HEAD_DIM
        lane = lax.broadcasted_iota(jnp.int32, (BLK, LANES), 1)
        live = lax.broadcasted_iota(jnp.int32, (2 * BLK, entries * BLK), 1) < count * BLK
        logs = jnp.zeros((BLK, LANES), jnp.float32)
        for pair in range(width // LANES):
            lanes = slice(pair * LANES, (pair + 1) * LANES)
            both = q_ref[rows, lanes]
            none = jnp.zeros_like(both)
            stacked = jnp.concatenate([jnp.where(first, both, none), jnp.where(first, none, both)], axis=0)
            scores = lax.dot_general(
                stacked, keys[:, lanes], (((1,), (1,)), ((), ())), preferred_element_type=jnp.float32
            )
            scores = jnp.where(live, scores, masked_score)
            top = jnp.max(scores, axis=1, keepdims=True)
            weights = jnp.exp(scores - top)
            total = jnp.sum(weights, axis=1, keepdims=True)
            summed = jnp.dot(
                weights.astype(jnp.bfloat16), values[:, lanes], preferred_element_type=jnp.float32
            )
            summed = summed / total
            out_ref[rows, lanes] = jnp.where(first, summed[:BLK], summed[BLK:]).astype(jnp.bfloat16)
            log_sum = top + jnp.log(total)
            logs = jnp.where(lane == 2 * pair, log_sum[:BLK], logs)
            logs = jnp.where(lane == 2 * pair + 1, log_sum[BLK:], logs)
        log_ref[rows, :] = logs
        return carry

    lax.fori_loop(0, blocks, one_block, 0)


def mix_kernel(n, att_ref, w_ref, out_ref, stage, landed, send_sem, recv_sem):
    me = lax.axis_index("tp")
    rows = out_ref.shape[0]
    tile = min(512, w_ref.shape[1])
    tiles = w_ref.shape[1] // tile
    peers = [lax.rem(me + d, n) for d in range(n)]
    barrier = pltpu.get_barrier_semaphore()
    for d in range(1, n):
        pl.semaphore_signal(barrier, inc=1, device_id={"tp": peers[d]}, device_id_type=pl.DeviceIdType.MESH)
    pl.semaphore_wait(barrier, n - 1)

    def partial_of(d, j):
        mine = att_ref[pl.ds(pl.multiple_of(peers[d] * rows, rows), rows), :]
        made = jnp.dot(mine, w_ref[:, j * tile : (j + 1) * tile], preferred_element_type=jnp.float32)
        return made.astype(jnp.bfloat16)

    def hop(d, j):
        return pltpu.make_async_remote_copy(
            src_ref=stage.at[d - 1, j],
            dst_ref=landed.at[d - 1, j],
            send_sem=send_sem.at[d - 1, j],
            recv_sem=recv_sem.at[d - 1, j],
            device_id={"tp": peers[d]},
            device_id_type=pl.DeviceIdType.MESH,
        )

    for d in range(1, n):
        for j in range(tiles):
            stage[d - 1, j] = partial_of(d, j)
            hop(d, j).start()
    for j in range(tiles):
        acc = partial_of(0, j).astype(jnp.float32)
        for d in range(1, n):
            hop(d, j).wait_recv()
            acc = acc + landed[d - 1, j].astype(jnp.float32)
        out_ref[:, j * tile : (j + 1) * tile] = acc.astype(jnp.bfloat16)
    for d in range(1, n):
        for j in range(tiles):
            hop(d, j).wait_send()


def local(devices, splits, tokens, w_query, w_key, w_value, w_out, chosen):
    rows, depth = tokens.shape
    width = w_query.shape[1]
    heads = width // HEAD_DIM
    blocks = rows // BLK
    group = 1
    while group * group < devices:
        group *= 2
    layers = devices // group
    all_blocks = chosen.shape[0]
    me = lax.axis_index("kv")

    half = HEAD_DIM // 2
    inverse = rotary_base ** (-jnp.arange(half, dtype=jnp.float32) / half)
    positions = (me * rows + jnp.arange(rows)).astype(jnp.float32)
    angles = positions[:, None] * inverse[None, :]
    cos_half, sin_half = jnp.cos(angles), jnp.sin(angles)
    cos_part = jnp.concatenate([cos_half] * (LANES // half), axis=1)
    sin_part = jnp.concatenate([-sin_half, sin_half] * (LANES // HEAD_DIM), axis=1)

    wide = min(2 * LANES, width)
    tiles = width // wide
    chunks = 2 * tiles
    kv, query = pl.pallas_call(
        functools.partial(project_kernel, tiles),
        grid=(3 * tiles,),
        in_specs=[
            pl.BlockSpec((rows, depth), lambda j: (0, 0)),
            pl.BlockSpec((depth, wide), lambda j: (0, jnp.minimum(j, tiles - 1))),
            pl.BlockSpec((depth, wide), lambda j: (0, jnp.clip(j - tiles, 0, tiles - 1))),
            pl.BlockSpec((depth, wide), lambda j: (0, jnp.maximum(j - 2 * tiles, 0))),
            pl.BlockSpec((rows, LANES), lambda j: (0, 0)),
            pl.BlockSpec((rows, LANES), lambda j: (0, 0)),
        ],
        out_specs=[
            pl.BlockSpec((1, rows, wide), lambda j: (jnp.minimum(j, chunks - 1), 0, 0)),
            pl.BlockSpec((rows, wide), lambda j: (0, jnp.maximum(j - chunks, 0))),
        ],
        out_shape=[
            jax.ShapeDtypeStruct((chunks, rows, wide), jnp.bfloat16),
            jax.ShapeDtypeStruct((rows, width), jnp.bfloat16),
        ],
        compiler_params=pltpu.CompilerParams(
            dimension_semantics=("arbitrary",), vmem_limit_bytes=VMEM_LIMIT
        ),
        name="project",
    )(tokens, w_key, w_value, w_query, cos_part, sin_part)

    flat = chosen.reshape(devices, -1)
    listed = jnp.any(flat[:, :, None] == jnp.arange(all_blocks)[None, None, :], axis=1)
    listed = listed.reshape(devices, devices, blocks).astype(jnp.int32)
    before = (jnp.arange(blocks)[:, None] < jnp.arange(blocks)[None, :]).astype(jnp.int32)
    slots = jnp.sum(listed[:, :, :, None] * before[None, None], axis=2)
    fits = (slots[:, :, None, :] == jnp.arange(CAP)[:, None]) & (listed[:, :, None, :] > 0)
    sel = jnp.sum(jnp.where(fits, jnp.arange(blocks), 0), axis=-1).reshape(devices, devices * CAP)
    slots = jnp.minimum(slots, CAP - 1).reshape(devices, all_blocks)

    table_rows = (layers * blocks + (group - 1) * layers * CAP) * BLK
    table = pl.pallas_call(
        functools.partial(exchange_kernel, layers, group, blocks),
        in_specs=[in_smem(), in_vmem()],
        out_specs=in_vmem(),
        out_shape=jax.ShapeDtypeStruct((chunks, table_rows, wide), jnp.bfloat16),
        scratch_shapes=[
            pltpu.VMEM((group - 1, layers, chunks, CAP * BLK, wide), jnp.bfloat16),
            pltpu.SemaphoreType.DMA((layers, chunks)),
            pltpu.SemaphoreType.DMA((layers, chunks)),
            pltpu.SemaphoreType.DMA((group - 1, layers, chunks)),
            pltpu.SemaphoreType.DMA((group - 1, layers, chunks)),
            pltpu.SemaphoreType.DMA,
        ],
        compiler_params=pltpu.CompilerParams(
            collective_id=0, has_side_effects=True, vmem_limit_bytes=VMEM_LIMIT
        ),
        name="exchange",
    )(sel, kv)

    attended, logs = pl.pallas_call(
        functools.partial(attend_kernel, layers, group, blocks),
        in_specs=[in_smem(), in_smem(), in_vmem(), in_vmem()],
        out_specs=[in_vmem(), in_vmem()],
        out_shape=[
            jax.ShapeDtypeStruct((rows, width), jnp.bfloat16),
            jax.ShapeDtypeStruct((rows, LANES), jnp.float32),
        ],
        scratch_shapes=[pltpu.VMEM((chosen.shape[1] * BLK, width), jnp.bfloat16)] * 2,
        compiler_params=pltpu.CompilerParams(vmem_limit_bytes=VMEM_LIMIT),
        name="attend",
    )(chosen, slots, query, table)
    log_sums = jnp.transpose(logs[:, :heads])

    out_rows = rows // splits
    tile = min(512, w_out.shape[1])
    out_tiles = w_out.shape[1] // tile
    output = pl.pallas_call(
        functools.partial(mix_kernel, splits),
        in_specs=[in_vmem(), in_vmem()],
        out_specs=in_vmem(),
        out_shape=jax.ShapeDtypeStruct((out_rows, w_out.shape[1]), jnp.bfloat16),
        scratch_shapes=[
            pltpu.VMEM((splits - 1, out_tiles, out_rows, tile), jnp.bfloat16),
            pltpu.VMEM((splits - 1, out_tiles, out_rows, tile), jnp.bfloat16),
            pltpu.SemaphoreType.DMA((splits - 1, out_tiles)),
            pltpu.SemaphoreType.DMA((splits - 1, out_tiles)),
        ],
        compiler_params=pltpu.CompilerParams(
            collective_id=1, has_side_effects=True, vmem_limit_bytes=VMEM_LIMIT
        ),
        name="mix",
    )(attended, w_out)
    return (output, log_sums)


def solution(mesh):
    placed = (P("kv", None), P(None, "tp"), P(None, "tp"), P(None, "tp"), P("tp", None), P())
    return jax.shard_map(
        functools.partial(local, mesh.shape["kv"], mesh.shape["tp"]),
        mesh=mesh,
        in_specs=placed,
        out_specs=(P(("kv", "tp"), None), P("tp", "kv")),
        check_vma=False,
    )
```

```python
import functools

import jax
import jax.numpy as jnp
from jax import lax
from jax.experimental import pallas as pl
from jax.experimental.pallas import tpu as pltpu
from jax.sharding import PartitionSpec as P

HEAD_DIM = 64
BLK = 64
CAP = 2
LANES = 128
VMEM_LIMIT = 48 * 1024 * 1024

rotary_base = 500000.0
masked_score = -1e30


def in_vmem():
    return pl.BlockSpec(memory_space=pltpu.VMEM)


def in_smem():
    return pl.BlockSpec(memory_space=pltpu.SMEM)


def attention_kernel(
    layers, group, blocks, places_ref, sel_ref, x_ref, wk_ref, wv_ref, wq_ref, cos_ref, sin_ref,
    out_ref, log_ref, wkv, wq, query, stage, picked, load_sem, col_send, col_recv, pl_send, pl_recv, *tables
):
    pairs = len(tables)
    entries = places_ref.shape[1] - 1
    me = lax.axis_index("kv")
    z = lax.div(me, group)
    g = lax.rem(me, group)
    up = lax.rem(me + group, layers * group)
    down = lax.rem(me + (layers - 1) * group, layers * group)
    half = HEAD_DIM // 2
    mesh_ids = pl.DeviceIdType.MESH
    peers = [z * group + lax.rem(g + d, group) for d in range(group)]

    def load(kind, ch):
        lanes = pl.ds(ch * LANES, LANES)
        source = (wk_ref, wv_ref, wq_ref)[kind].at[:, lanes]
        if kind < 2:
            target = wkv.at[ch, :, pl.ds(kind * LANES, LANES)]
        else:
            target = wq.at[:, lanes]
        return pltpu.make_async_copy(source, target, load_sem.at[kind, ch])

    for ch in range(pairs):
        load(0, ch).start()
        load(1, ch).start()
    for ch in range(pairs):
        load(2, ch).start()

    barrier = pltpu.get_barrier_semaphore()
    for d in range(1, group):
        pl.semaphore_signal(barrier, inc=1, device_id={"kv": peers[d]}, device_id_type=mesh_ids)

    @pl.when(z < layers - 1)
    def _():
        pl.semaphore_signal(barrier, inc=1, device_id={"kv": up}, device_id_type=mesh_ids)

    @pl.when(z > 0)
    def _():
        pl.semaphore_signal(barrier, inc=1, device_id={"kv": down}, device_id_type=mesh_ids)

    def column_copy(t, ch):
        return pltpu.make_async_remote_copy(
            src_ref=tables[ch].at[pl.ds(t * blocks, blocks)],
            dst_ref=tables[ch].at[pl.ds((t + 1) * blocks, blocks)],
            send_sem=col_send.at[t, ch],
            recv_sem=col_recv.at[t, ch],
            device_id={"kv": up},
            device_id_type=mesh_ids,
        )

    def plane_copy(d, t, ch):
        place = layers * blocks + ((d - 1) * layers + t) * CAP
        return pltpu.make_async_remote_copy(
            src_ref=stage.at[d - 1, t, ch],
            dst_ref=tables[ch].at[pl.ds(place, CAP)],
            send_sem=pl_send.at[d - 1, t, ch],
            recv_sem=pl_recv.at[d - 1, t, ch],
            device_id={"kv": peers[d]},
            device_id_type=mesh_ids,
        )

    def hand_on(d, t, ch):
        for c in range(CAP):
            index = sel_ref[peers[d], ((z - t) * group + g) * CAP + c]
            chosen_tile = None
            for i in range(blocks):
                tile = tables[ch][t * blocks + i]
                chosen_tile = tile if chosen_tile is None else jnp.where(index == i, tile, chosen_tile)
            stage[d - 1, t, ch, c] = chosen_tile
        plane_copy(d, t, ch).start()

    def send_set(t, ch):
        if t < layers - 1:

            @pl.when(z < layers - 1)
            def _():
                column_copy(t, ch).start()

        for d in range(1, group):
            if t == 0:
                pl.when(g + d < group)(functools.partial(hand_on, d, t, ch))
            else:
                hand_on(d, t, ch)

    cos_part = cos_ref[...]
    sin_part = sin_ref[...]
    low = lax.broadcasted_iota(jnp.int32, cos_part.shape, 1) % HEAD_DIM < half

    def turned(part):
        other = jnp.where(low, pltpu.roll(part, LANES - half, 1), pltpu.roll(part, half, 1))
        return part * cos_part + other * sin_part

    for ch in range(pairs):
        load(0, ch).wait()
        load(1, ch).wait()
        made = jnp.dot(x_ref[...], wkv[ch], preferred_element_type=jnp.float32)
        key_rows = turned(made[:, :LANES]).astype(jnp.bfloat16)
        value_rows = made[:, LANES:].astype(jnp.bfloat16)
        for i in range(blocks):
            tables[ch][i, :, :LANES] = key_rows[i * BLK : (i + 1) * BLK]
            tables[ch][i, :, LANES:] = value_rows[i * BLK : (i + 1) * BLK]
        if ch == 0:
            pl.semaphore_wait(barrier, group - 1 + jnp.minimum(z, 1) + jnp.minimum(layers - 1 - z, 1))
        send_set(0, ch)

    for ch in range(pairs):
        load(2, ch).wait()
    wide = min(2 * LANES, pairs * LANES)
    for lane in range(0, pairs * LANES, wide):
        made = jnp.dot(x_ref[...], wq[:, lane : lane + wide], preferred_element_type=jnp.float32)
        for part in range(0, wide, LANES):
            piece = turned(made[:, part : part + LANES]).astype(jnp.bfloat16)
            query[:, lane + part : lane + part + LANES] = (piece * (HEAD_DIM**-0.5)).astype(jnp.bfloat16)

    first = lax.broadcasted_iota(jnp.int32, (BLK, LANES), 1) < HEAD_DIM
    lane_index = lax.broadcasted_iota(jnp.int32, (BLK, LANES), 1)

    def attend(ch):
        lanes = slice(ch * LANES, (ch + 1) * LANES)

        def one_block(r, carry):
            count = places_ref[r, entries]
            for s in range(entries):
                picked[s * BLK : (s + 1) * BLK, :] = tables[ch][places_ref[r, s]]
            rows = pl.ds(pl.multiple_of(r * BLK, BLK), BLK)
            live = lax.broadcasted_iota(jnp.int32, (2 * BLK, entries * BLK), 1) < count * BLK
            both = query[rows, lanes]
            none = jnp.zeros_like(both)
            stacked = jnp.concatenate([jnp.where(first, both, none), jnp.where(first, none, both)], axis=0)
            scores = lax.dot_general(
                stacked, picked[:, :LANES], (((1,), (1,)), ((), ())), preferred_element_type=jnp.float32
            )
            scores = jnp.where(live, scores, masked_score)
            top = jnp.max(scores, axis=1, keepdims=True)
            weights = jnp.exp(scores - top)
            total = jnp.sum(weights, axis=1, keepdims=True)
            summed = jnp.dot(
                weights.astype(jnp.bfloat16), picked[:, LANES:], preferred_element_type=jnp.float32
            )
            summed = summed / total
            out_ref[rows, lanes] = jnp.where(first, summed[:BLK], summed[BLK:]).astype(jnp.bfloat16)
            log_sum = top + jnp.log(total)
            logs = jnp.zeros((BLK, LANES), jnp.float32) if ch == 0 else log_ref[rows, :]
            logs = jnp.where(lane_index == 2 * ch, log_sum[:BLK], logs)
            log_ref[rows, :] = jnp.where(lane_index == 2 * ch + 1, log_sum[BLK:], logs)
            return carry

        lax.fori_loop(0, blocks, one_block, 0)

    def finish(ch):
        for t in range(layers):

            @pl.when(z >= t)
            def _():
                for d in range(1, group):
                    if t == 0:
                        pl.when(g >= d)(lambda d=d: plane_copy(d, t, ch).wait_recv())
                    else:
                        plane_copy(d, t, ch).wait_recv()

        attend(ch)

    for ch in range(pairs):
        for t in range(1, layers):

            @pl.when(z >= t)
            def _():
                column_copy(t - 1, ch).wait_recv()
                send_set(t, ch)

        if ch > 0:
            finish(ch - 1)
    finish(pairs - 1)

    for ch in range(pairs):
        for t in range(layers):

            @pl.when(z >= t)
            def _():
                if t < layers - 1:

                    @pl.when(z < layers - 1)
                    def _():
                        column_copy(t, ch).wait_send()

                for d in range(1, group):
                    if t == 0:
                        pl.when(g + d < group)(lambda d=d: plane_copy(d, t, ch).wait_send())
                    else:
                        plane_copy(d, t, ch).wait_send()


def mix_kernel(n, att_ref, w_ref, out_ref, stage, landed, send_sem, recv_sem):
    me = lax.axis_index("tp")
    rows = out_ref.shape[0]
    tile = min(512, w_ref.shape[1])
    tiles = w_ref.shape[1] // tile
    peers = [lax.rem(me + d, n) for d in range(n)]
    barrier = pltpu.get_barrier_semaphore()
    for d in range(1, n):
        pl.semaphore_signal(barrier, inc=1, device_id={"tp": peers[d]}, device_id_type=pl.DeviceIdType.MESH)
    pl.semaphore_wait(barrier, n - 1)

    def partial_of(d, j):
        mine = att_ref[pl.ds(pl.multiple_of(peers[d] * rows, rows), rows), :]
        made = jnp.dot(mine, w_ref[:, j * tile : (j + 1) * tile], preferred_element_type=jnp.float32)
        return made.astype(jnp.bfloat16)

    def hop(d, j):
        return pltpu.make_async_remote_copy(
            src_ref=stage.at[d - 1, j],
            dst_ref=landed.at[d - 1, j],
            send_sem=send_sem.at[d - 1, j],
            recv_sem=recv_sem.at[d - 1, j],
            device_id={"tp": peers[d]},
            device_id_type=pl.DeviceIdType.MESH,
        )

    for d in range(1, n):
        for j in range(tiles):
            stage[d - 1, j] = partial_of(d, j)
            hop(d, j).start()
    for j in range(tiles):
        acc = partial_of(0, j).astype(jnp.float32)
        for d in range(1, n):
            hop(d, j).wait_recv()
            acc = acc + landed[d - 1, j].astype(jnp.float32)
        out_ref[:, j * tile : (j + 1) * tile] = acc.astype(jnp.bfloat16)
    for d in range(1, n):
        for j in range(tiles):
            hop(d, j).wait_send()


def local(devices, splits, tokens, w_query, w_key, w_value, w_out, chosen):
    rows, depth = tokens.shape
    width = w_query.shape[1]
    heads = width // HEAD_DIM
    blocks = rows // BLK
    group = 1
    while group * group < devices:
        group *= 2
    layers = devices // group
    all_blocks = chosen.shape[0]
    me = lax.axis_index("kv")

    half = HEAD_DIM // 2
    inverse = rotary_base ** (-jnp.arange(half, dtype=jnp.float32) / half)
    positions = (me * rows + jnp.arange(rows)).astype(jnp.float32)
    angles = positions[:, None] * inverse[None, :]
    cos_half, sin_half = jnp.cos(angles), jnp.sin(angles)
    cos_part = jnp.concatenate([cos_half] * (LANES // half), axis=1)
    sin_part = jnp.concatenate([-sin_half, sin_half] * (LANES // HEAD_DIM), axis=1)

    flat = chosen.reshape(devices, -1)
    listed = jnp.any(flat[:, :, None] == jnp.arange(all_blocks)[None, None, :], axis=1)
    listed = listed.reshape(devices, devices, blocks).astype(jnp.int32)
    before = (jnp.arange(blocks)[:, None] < jnp.arange(blocks)[None, :]).astype(jnp.int32)
    slots = jnp.sum(listed[:, :, :, None] * before[None, None], axis=2)
    fits = (slots[:, :, None, :] == jnp.arange(CAP)[:, None]) & (listed[:, :, None, :] > 0)
    sel = jnp.sum(jnp.where(fits, jnp.arange(blocks), 0), axis=-1).reshape(devices, devices * CAP)

    own_lists = lax.dynamic_slice_in_dim(chosen, me * blocks, blocks, 0)
    own_slots = lax.dynamic_slice_in_dim(slots.reshape(devices, all_blocks), me, 1, 0)
    own_blocks = jnp.where(own_lists >= 0, own_lists, me * blocks + jnp.arange(blocks)[:, None])
    every_block = jnp.arange(all_blocks)
    owners = every_block // blocks
    steps = me // group - owners // group
    across = (me % group - owners % group + group) % group
    handed = layers * blocks + ((across - 1) * layers + steps) * CAP + jnp.minimum(own_slots[0], CAP - 1)
    home = jnp.where(across == 0, steps * blocks + every_block % blocks, handed)
    places = jnp.sum(jnp.where(own_blocks[:, :, None] == every_block, home, 0), axis=-1)
    counts = jnp.sum((own_lists >= 0).astype(jnp.int32), axis=1, keepdims=True)
    places = jnp.concatenate([places, counts], axis=1)

    table_blocks = layers * blocks + (group - 1) * layers * CAP
    pairs = width // LANES
    in_hbm = pl.BlockSpec(memory_space=pltpu.HBM)
    attended, logs = pl.pallas_call(
        functools.partial(attention_kernel, layers, group, blocks),
        in_specs=[in_smem()] * 2 + [in_vmem()] + [in_hbm] * 3 + [in_vmem()] * 2,
        out_specs=[in_vmem(), in_vmem()],
        out_shape=[
            jax.ShapeDtypeStruct((rows, width), jnp.bfloat16),
            jax.ShapeDtypeStruct((rows, LANES), jnp.float32),
        ],
        scratch_shapes=[
            pltpu.VMEM((pairs, depth, 2 * LANES), jnp.bfloat16),
            pltpu.VMEM((depth, width), jnp.bfloat16),
            pltpu.VMEM((rows, width), jnp.bfloat16),
            pltpu.VMEM((group - 1, layers, pairs, CAP, BLK, 2 * LANES), jnp.bfloat16),
            pltpu.VMEM((chosen.shape[1] * BLK, 2 * LANES), jnp.bfloat16),
            pltpu.SemaphoreType.DMA((3, pairs)),
            pltpu.SemaphoreType.DMA((layers, pairs)),
            pltpu.SemaphoreType.DMA((layers, pairs)),
            pltpu.SemaphoreType.DMA((group - 1, layers, pairs)),
            pltpu.SemaphoreType.DMA((group - 1, layers, pairs)),
        ]
        + [pltpu.VMEM((table_blocks, BLK, 2 * LANES), jnp.bfloat16)] * pairs,
        compiler_params=pltpu.CompilerParams(
            collective_id=0, has_side_effects=True, vmem_limit_bytes=VMEM_LIMIT
        ),
        name="attention",
    )(places, sel, tokens, w_key, w_value, w_query, cos_part, sin_part)
    log_sums = jnp.transpose(logs[:, :heads])

    out_rows = rows // splits
    tile = min(512, w_out.shape[1])
    out_tiles = w_out.shape[1] // tile
    output = pl.pallas_call(
        functools.partial(mix_kernel, splits),
        in_specs=[in_vmem(), in_vmem()],
        out_specs=in_vmem(),
        out_shape=jax.ShapeDtypeStruct((out_rows, w_out.shape[1]), jnp.bfloat16),
        scratch_shapes=[
            pltpu.VMEM((splits - 1, out_tiles, out_rows, tile), jnp.bfloat16),
            pltpu.VMEM((splits - 1, out_tiles, out_rows, tile), jnp.bfloat16),
            pltpu.SemaphoreType.DMA((splits - 1, out_tiles)),
            pltpu.SemaphoreType.DMA((splits - 1, out_tiles)),
        ],
        compiler_params=pltpu.CompilerParams(
            collective_id=1, has_side_effects=True, vmem_limit_bytes=VMEM_LIMIT
        ),
        name="mix",
    )(attended, w_out)
    return (output, log_sums)


def solution(mesh):
    placed = (P("kv", None), P(None, "tp"), P(None, "tp"), P(None, "tp"), P("tp", None), P())
    return jax.shard_map(
        functools.partial(local, mesh.shape["kv"], mesh.shape["tp"]),
        mesh=mesh,
        in_specs=placed,
        out_specs=(P(("kv", "tp"), None), P("tp", "kv")),
        check_vma=False,
    )
```

```python
import functools

import jax
import jax.numpy as jnp
from jax import lax
from jax.experimental import pallas as pl
from jax.experimental.pallas import tpu as pltpu
from jax.sharding import PartitionSpec as P

HEAD_DIM = 64
BLK = 64
CAP = 2
LANES = 128
VMEM_LIMIT = 62 * 1024 * 1024

rotary_base = 500000.0
masked_score = -1e30


def in_vmem():
    return pl.BlockSpec(memory_space=pltpu.VMEM)


def in_smem():
    return pl.BlockSpec(memory_space=pltpu.SMEM)


def attention_kernel(
    layers, group, blocks, splits, places_ref, sel_ref, tokens_ref, wk_ref, wv_ref, wq_ref, wo_ref, cos_ref, sin_ref,
    mixed_ref, log_ref, x_ref, wo, out_ref, part_stage, landed, part_send, part_recv, side_sem, wkv, wq, query, stage, picked, load_sem, col_send, col_recv, pl_send, pl_recv, *tables
):
    pairs = len(tables)
    entries = places_ref.shape[1] - 1
    me = lax.axis_index("kv")
    z = lax.div(me, group)
    g = lax.rem(me, group)
    up = lax.rem(me + group, layers * group)
    down = lax.rem(me + (layers - 1) * group, layers * group)
    half = HEAD_DIM // 2
    mesh_ids = pl.DeviceIdType.MESH
    peers = [z * group + lax.rem(g + d, group) for d in range(group)]

    def load(kind, ch):
        lanes = pl.ds(ch * LANES, LANES)
        source = (wk_ref, wv_ref, wq_ref)[kind].at[:, lanes]
        if kind < 2:
            target = wkv.at[ch, :, pl.ds(kind * LANES, LANES)]
        else:
            target = wq.at[:, lanes]
        return pltpu.make_async_copy(source, target, load_sem.at[kind, ch])

    token_load = pltpu.make_async_copy(tokens_ref, x_ref, side_sem.at[0])
    out_load = pltpu.make_async_copy(wo_ref, wo, side_sem.at[1])
    token_load.start()
    for ch in range(pairs):
        load(0, ch).start()
        load(1, ch).start()
    for ch in range(pairs):
        load(2, ch).start()
    out_load.start()

    barrier = pltpu.get_barrier_semaphore()
    side = lax.axis_index("tp")
    others = [lax.rem(side + d, splits) for d in range(splits)]
    for d in range(1, splits):
        pl.semaphore_signal(barrier, inc=1, device_id={"tp": others[d]}, device_id_type=mesh_ids)
    for d in range(1, group):
        pl.semaphore_signal(barrier, inc=1, device_id={"kv": peers[d]}, device_id_type=mesh_ids)

    @pl.when(z < layers - 1)
    def _():
        pl.semaphore_signal(barrier, inc=1, device_id={"kv": up}, device_id_type=mesh_ids)

    @pl.when(z > 0)
    def _():
        pl.semaphore_signal(barrier, inc=1, device_id={"kv": down}, device_id_type=mesh_ids)

    def column_copy(t, ch):
        return pltpu.make_async_remote_copy(
            src_ref=tables[ch].at[pl.ds(t * blocks, blocks)],
            dst_ref=tables[ch].at[pl.ds((t + 1) * blocks, blocks)],
            send_sem=col_send.at[t, ch],
            recv_sem=col_recv.at[t, ch],
            device_id={"kv": up},
            device_id_type=mesh_ids,
        )

    def plane_copy(d, t, ch):
        place = layers * blocks + ((d - 1) * layers + t) * CAP
        return pltpu.make_async_remote_copy(
            src_ref=stage.at[d - 1, t, ch],
            dst_ref=tables[ch].at[pl.ds(place, CAP)],
            send_sem=pl_send.at[d - 1, t, ch],
            recv_sem=pl_recv.at[d - 1, t, ch],
            device_id={"kv": peers[d]},
            device_id_type=mesh_ids,
        )

    def hand_on(d, t, ch):
        for c in range(CAP):
            index = sel_ref[peers[d], ((z - t) * group + g) * CAP + c]
            chosen_tile = None
            for i in range(blocks):
                tile = tables[ch][t * blocks + i]
                chosen_tile = tile if chosen_tile is None else jnp.where(index == i, tile, chosen_tile)
            stage[d - 1, t, ch, c] = chosen_tile
        plane_copy(d, t, ch).start()

    def send_set(t, ch):
        if t < layers - 1:

            @pl.when(z < layers - 1)
            def _():
                column_copy(t, ch).start()

        for d in range(1, group):
            if t == 0:
                pl.when(g + d < group)(functools.partial(hand_on, d, t, ch))
            else:
                hand_on(d, t, ch)

    cos_part = cos_ref[...]
    sin_part = sin_ref[...]
    low = lax.broadcasted_iota(jnp.int32, cos_part.shape, 1) % HEAD_DIM < half

    def turned(part):
        other = jnp.where(low, pltpu.roll(part, LANES - half, 1), pltpu.roll(part, half, 1))
        return part * cos_part + other * sin_part

    token_load.wait()
    for ch in range(pairs):
        load(0, ch).wait()
        load(1, ch).wait()
        made = jnp.dot(x_ref[...], wkv[ch], preferred_element_type=jnp.float32)
        key_rows = turned(made[:, :LANES]).astype(jnp.bfloat16)
        value_rows = made[:, LANES:].astype(jnp.bfloat16)
        for i in range(blocks):
            tables[ch][i, :, :LANES] = key_rows[i * BLK : (i + 1) * BLK]
            tables[ch][i, :, LANES:] = value_rows[i * BLK : (i + 1) * BLK]
        if ch == 0:
            pl.semaphore_wait(barrier, splits + group - 2 + jnp.minimum(z, 1) + jnp.minimum(layers - 1 - z, 1))
        send_set(0, ch)

    for ch in range(pairs):
        load(2, ch).wait()
    wide = min(2 * LANES, pairs * LANES)
    for lane in range(0, pairs * LANES, wide):
        made = jnp.dot(x_ref[...], wq[:, lane : lane + wide], preferred_element_type=jnp.float32)
        for part in range(0, wide, LANES):
            piece = turned(made[:, part : part + LANES]).astype(jnp.bfloat16)
            query[:, lane + part : lane + part + LANES] = (piece * (HEAD_DIM**-0.5)).astype(jnp.bfloat16)

    first = lax.broadcasted_iota(jnp.int32, (BLK, LANES), 1) < HEAD_DIM
    lane_index = lax.broadcasted_iota(jnp.int32, (BLK, LANES), 1)

    def attend(ch):
        lanes = slice(ch * LANES, (ch + 1) * LANES)

        def one_block(r, carry):
            count = places_ref[r, entries]
            for s in range(entries):
                picked[s * BLK : (s + 1) * BLK, :] = tables[ch][places_ref[r, s]]
            rows = pl.ds(pl.multiple_of(r * BLK, BLK), BLK)
            live = lax.broadcasted_iota(jnp.int32, (2 * BLK, entries * BLK), 1) < count * BLK
            both = query[rows, lanes]
            none = jnp.zeros_like(both)
            stacked = jnp.concatenate([jnp.where(first, both, none), jnp.where(first, none, both)], axis=0)
            scores = lax.dot_general(
                stacked, picked[:, :LANES], (((1,), (1,)), ((), ())), preferred_element_type=jnp.float32
            )
            scores = jnp.where(live, scores, masked_score)
            top = jnp.max(scores, axis=1, keepdims=True)
            weights = jnp.exp(scores - top)
            total = jnp.sum(weights, axis=1, keepdims=True)
            summed = jnp.dot(
                weights.astype(jnp.bfloat16), picked[:, LANES:], preferred_element_type=jnp.float32
            )
            summed = summed / total
            out_ref[rows, lanes] = jnp.where(first, summed[:BLK], summed[BLK:]).astype(jnp.bfloat16)
            log_sum = top + jnp.log(total)
            logs = jnp.zeros((BLK, LANES), jnp.float32) if ch == 0 else log_ref[rows, :]
            logs = jnp.where(lane_index == 2 * ch, log_sum[:BLK], logs)
            log_ref[rows, :] = jnp.where(lane_index == 2 * ch + 1, log_sum[BLK:], logs)
            return carry

        lax.fori_loop(0, blocks, one_block, 0)

    def finish(ch):
        for t in range(layers):

            @pl.when(z >= t)
            def _():
                for d in range(1, group):
                    if t == 0:
                        pl.when(g >= d)(lambda d=d: plane_copy(d, t, ch).wait_recv())
                    else:
                        plane_copy(d, t, ch).wait_recv()

        attend(ch)

    for ch in range(pairs):
        for t in range(1, layers):

            @pl.when(z >= t)
            def _():
                column_copy(t - 1, ch).wait_recv()
                send_set(t, ch)

        if ch > 0:
            finish(ch - 1)
    finish(pairs - 1)

    for ch in range(pairs):
        for t in range(layers):

            @pl.when(z >= t)
            def _():
                if t < layers - 1:

                    @pl.when(z < layers - 1)
                    def _():
                        column_copy(t, ch).wait_send()

                for d in range(1, group):
                    if t == 0:
                        pl.when(g + d < group)(lambda d=d: plane_copy(d, t, ch).wait_send())
                    else:
                        plane_copy(d, t, ch).wait_send()

    rows_out = mixed_ref.shape[0]
    tile = min(512, wo.shape[1])
    tiles = wo.shape[1] // tile
    out_load.wait()

    def partial_of(d, j):
        mine = out_ref[pl.ds(pl.multiple_of(others[d] * rows_out, rows_out), rows_out), :]
        made = jnp.dot(mine, wo[:, j * tile : (j + 1) * tile], preferred_element_type=jnp.float32)
        return made.astype(jnp.bfloat16)

    def hop(d, j):
        return pltpu.make_async_remote_copy(
            src_ref=part_stage.at[d - 1, j],
            dst_ref=landed.at[d - 1, j],
            send_sem=part_send.at[d - 1, j],
            recv_sem=part_recv.at[d - 1, j],
            device_id={"tp": others[d]},
            device_id_type=mesh_ids,
        )

    for d in range(1, splits):
        for j in range(tiles):
            part_stage[d - 1, j] = partial_of(d, j)
            hop(d, j).start()
    for j in range(tiles):
        acc = partial_of(0, j).astype(jnp.float32)
        for d in range(1, splits):
            hop(d, j).wait_recv()
            acc = acc + landed[d - 1, j].astype(jnp.float32)
        mixed_ref[:, j * tile : (j + 1) * tile] = acc.astype(jnp.bfloat16)
    for d in range(1, splits):
        for j in range(tiles):
            hop(d, j).wait_send()


def local(devices, splits, tokens, w_query, w_key, w_value, w_out, chosen):
    rows, depth = tokens.shape
    width = w_query.shape[1]
    heads = width // HEAD_DIM
    blocks = rows // BLK
    group = 1
    while group * group < devices:
        group *= 2
    layers = devices // group
    all_blocks = chosen.shape[0]
    me = lax.axis_index("kv")

    half = HEAD_DIM // 2
    inverse = rotary_base ** (-jnp.arange(half, dtype=jnp.float32) / half)
    positions = (me * rows + jnp.arange(rows)).astype(jnp.float32)
    angles = positions[:, None] * inverse[None, :]
    cos_half, sin_half = jnp.cos(angles), jnp.sin(angles)
    cos_part = jnp.concatenate([cos_half] * (LANES // half), axis=1)
    sin_part = jnp.concatenate([-sin_half, sin_half] * (LANES // HEAD_DIM), axis=1)

    flat = chosen.reshape(devices, -1)
    listed = jnp.any(flat[:, :, None] == jnp.arange(all_blocks)[None, None, :], axis=1)
    listed = listed.reshape(devices, devices, blocks).astype(jnp.int32)
    before = (jnp.arange(blocks)[:, None] < jnp.arange(blocks)[None, :]).astype(jnp.int32)
    slots = jnp.sum(listed[:, :, :, None] * before[None, None], axis=2)
    fits = (slots[:, :, None, :] == jnp.arange(CAP)[:, None]) & (listed[:, :, None, :] > 0)
    sel = jnp.sum(jnp.where(fits, jnp.arange(blocks), 0), axis=-1).reshape(devices, devices * CAP)

    own_lists = lax.dynamic_slice_in_dim(chosen, me * blocks, blocks, 0)
    own_slots = lax.dynamic_slice_in_dim(slots.reshape(devices, all_blocks), me, 1, 0)
    own_blocks = jnp.where(own_lists >= 0, own_lists, me * blocks + jnp.arange(blocks)[:, None])
    every_block = jnp.arange(all_blocks)
    owners = every_block // blocks
    steps = me // group - owners // group
    across = (me % group - owners % group + group) % group
    handed = layers * blocks + ((across - 1) * layers + steps) * CAP + jnp.minimum(own_slots[0], CAP - 1)
    home = jnp.where(across == 0, steps * blocks + every_block % blocks, handed)
    places = jnp.sum(jnp.where(own_blocks[:, :, None] == every_block, home, 0), axis=-1)
    counts = jnp.sum((own_lists >= 0).astype(jnp.int32), axis=1, keepdims=True)
    places = jnp.concatenate([places, counts], axis=1)

    table_blocks = layers * blocks + (group - 1) * layers * CAP
    pairs = width // LANES
    in_hbm = pl.BlockSpec(memory_space=pltpu.HBM)
    out_width = w_out.shape[1]
    out_rows = rows // splits
    tile = min(512, out_width)
    parts = (splits - 1, out_width // tile)
    output, logs = pl.pallas_call(
        functools.partial(attention_kernel, layers, group, blocks, splits),
        in_specs=[in_smem()] * 2 + [in_hbm] * 5 + [in_vmem()] * 2,
        out_specs=[in_vmem(), in_vmem()],
        out_shape=[
            jax.ShapeDtypeStruct((out_rows, out_width), jnp.bfloat16),
            jax.ShapeDtypeStruct((rows, LANES), jnp.float32),
        ],
        scratch_shapes=[
            pltpu.VMEM((rows, depth), jnp.bfloat16),
            pltpu.VMEM((width, out_width), jnp.bfloat16),
            pltpu.VMEM((rows, width), jnp.bfloat16),
            pltpu.VMEM(parts + (out_rows, tile), jnp.bfloat16),
            pltpu.VMEM(parts + (out_rows, tile), jnp.bfloat16),
            pltpu.SemaphoreType.DMA(parts),
            pltpu.SemaphoreType.DMA(parts),
            pltpu.SemaphoreType.DMA((2,)),
            pltpu.VMEM((pairs, depth, 2 * LANES), jnp.bfloat16),
            pltpu.VMEM((depth, width), jnp.bfloat16),
            pltpu.VMEM((rows, width), jnp.bfloat16),
            pltpu.VMEM((group - 1, layers, pairs, CAP, BLK, 2 * LANES), jnp.bfloat16),
            pltpu.VMEM((chosen.shape[1] * BLK, 2 * LANES), jnp.bfloat16),
            pltpu.SemaphoreType.DMA((3, pairs)),
            pltpu.SemaphoreType.DMA((layers, pairs)),
            pltpu.SemaphoreType.DMA((layers, pairs)),
            pltpu.SemaphoreType.DMA((group - 1, layers, pairs)),
            pltpu.SemaphoreType.DMA((group - 1, layers, pairs)),
        ]
        + [pltpu.VMEM((table_blocks, BLK, 2 * LANES), jnp.bfloat16)] * pairs,
        compiler_params=pltpu.CompilerParams(
            collective_id=0, has_side_effects=True, vmem_limit_bytes=VMEM_LIMIT
        ),
        name="attention",
    )(places, sel, tokens, w_key, w_value, w_query, w_out, cos_part, sin_part)
    log_sums = jnp.transpose(logs[:, :heads])

    return (output, log_sums)


def solution(mesh):
    placed = (P("kv", None), P(None, "tp"), P(None, "tp"), P(None, "tp"), P("tp", None), P())
    return jax.shard_map(
        functools.partial(local, mesh.shape["kv"], mesh.shape["tp"]),
        mesh=mesh,
        in_specs=placed,
        out_specs=(P(("kv", "tp"), None), P("tp", "kv")),
        check_vma=False,
    )
```
